32 devices in a mesh: fs: 8 (over z, x), tp: 4 (over y, core).
Axes of the slice: x: 2, y: 2, z: 4, core: 2. Of those that a mesh axis runs over, the one named last changes fastest.
Arguments:
- tokens: bfloat16 [16, 384, 2048], P('fs', None, 'tp'), may hold values from -20 to 20
- first_gain: float32 [2048], replicated, may hold values from 0.1 to 1.9
- first_gate: bfloat16 [2048, 5120], P('fs', 'tp'), may hold values from -0.125 to 0.125
- first_up: bfloat16 [2048, 5120], P('fs', 'tp'), may hold values from -0.125 to 0.125
- first_down: bfloat16 [5120, 2048], P('tp', 'fs'), may hold values from -0.078125 to 0.078125
- mixer_gain: float32 [2048], replicated, may hold values from 0.1 to 1.9
- conv_input: bfloat16 [2048, 1024], P('fs', 'tp'), may hold values from -0.125 to 0.125
- outer_gate: bfloat16 [2048, 1024], P('fs', 'tp'), may hold values from -0.125 to 0.125
- inner_gate: bfloat16 [2048, 1024], P('fs', 'tp'), may hold values from -0.125 to 0.125
- conv_taps: float32 [3, 1024], P(None, 'tp'), may hold values from -3.5 to 3.5
- mixer_out: bfloat16 [1024, 2048], P('tp', 'fs'), may hold values from -0.1875 to 0.1875
- second_gain: float32 [2048], replicated, may hold values from 0.1 to 1.9
- second_gate: bfloat16 [2048, 5120], P('fs', 'tp'), may hold values from -0.125 to 0.125
- second_up: bfloat16 [2048, 5120], P('fs', 'tp'), may hold values from -0.125 to 0.125
- second_down: bfloat16 [5120, 2048], P('tp', 'fs'), may hold values from -0.078125 to 0.078125
Outputs:
- layer_out: bfloat16 [16, 384, 2048], P('fs', None, 'tp')
The draws below stay inside these ranges and needn't reach their ends.
All inputs are finite; a program needn't handle non-finite values.
Results may differ from the reference program's by a relative error of at most 0.015.
Values may be sent and summed in bfloat16 or wider, within the bound.
A program may use at most 64 MiB of HBM per device.

```python
import jax
import jax.numpy as jnp
from jax import lax

D = 2048
FF = 5120
CW = 1024
KERNEL = 3
LEN = 384
SEQS = 16
N_TP = 4


def draw_tokens(key, part):
    key_base, key_block, key_scale = jax.random.split(key, 3)
    blocks = jax.random.uniform(key_block, (SEQS, LEN, N_TP, 1), jnp.float32, -1.1, 1.1)
    base = jnp.clip(jax.random.normal(key_base, (SEQS, LEN, N_TP, D // N_TP), jnp.float32), -6.0, 6.0)
    return (base * jnp.exp(blocks)).reshape(SEQS, LEN, D).astype(jnp.bfloat16)


def block_scale(key, extent, cuts, low, top_value):
    loudness = 1.0
    for axis_at, shards_of in cuts:
        draws = jax.random.uniform(jax.random.fold_in(jax.random.fold_in(key, 6), axis_at), (shards_of,), jnp.float32, low / len(cuts), top_value / len(cuts))
        loudness = loudness * jnp.repeat(jnp.exp(draws), extent[axis_at] // shards_of).reshape((-1,) + (1,) * (len(extent) - 1 - axis_at))
    return loudness


def normal_values(stream_key, dims, scale, bound, shards=(), held_as=jnp.bfloat16):
    result = jax.random.normal(stream_key, dims, jnp.float32) * scale
    if len(shards) > 0:
        result = block_scale(stream_key, dims, shards, -0.22, 0.18) * result
    return jnp.clip(result, min=-bound, max=bound).astype(held_as)


def setup_inputs(seed: int = 0) -> dict:
    keys = jax.random.split(jax.random.key(seed), 16)
    return {
        "tokens": draw_tokens(jax.random.fold_in(keys[15], 71), 0),
        "first_gain": jnp.clip(1.0 + 0.18 * jax.random.normal(keys[1], (D,), jnp.float32), 0.1, 1.9),
        "first_gate": normal_values(keys[2], (D, FF), D ** -0.5, 0.125, ((0, 8), (1, 4))),
        "first_up": normal_values(keys[3], (D, FF), D ** -0.5, 0.125, ((0, 8), (1, 4))),
        "first_down": normal_values(keys[4], (FF, D), FF ** -0.5, 0.078125, ((0, 4), (1, 8))),
        "mixer_gain": jnp.clip(1.0 + 0.18 * jax.random.normal(keys[5], (D,), jnp.float32), 0.1, 1.9),
        "conv_input": normal_values(keys[6], (D, CW), D ** -0.5, 0.125, ((0, 8), (1, 4))),
        "outer_gate": normal_values(keys[7], (D, CW), D ** -0.5, 0.125, ((0, 8), (1, 4))),
        "inner_gate": normal_values(keys[8], (D, CW), D ** -0.5, 0.125, ((0, 8), (1, 4))),
        "conv_taps": normal_values(keys[9], (KERNEL, CW), KERNEL ** -0.5, 3.5, ((1, 4),), jnp.float32),
        "mixer_out": normal_values(keys[10], (CW, D), CW ** -0.5, 0.1875, ((0, 4), (1, 8))),
        "second_gain": jnp.clip(1.0 + 0.18 * jax.random.normal(keys[11], (D,), jnp.float32), 0.1, 1.9),
        "second_gate": normal_values(keys[12], (D, FF), D ** -0.5, 0.125, ((0, 8), (1, 4))),
        "second_up": normal_values(keys[13], (D, FF), D ** -0.5, 0.125, ((0, 8), (1, 4))),
        "second_down": normal_values(keys[14], (FF, D), FF ** -0.5, 0.078125, ((0, 4), (1, 8))),
    }


epsilon = 1e-05

def norm_rows(stream, gain):
    values = stream.astype(jnp.float32)
    scale = lax.rsqrt(lax.optimization_barrier(jnp.mean(values * values, axis=1, keepdims=True)) + epsilon)
    return (values * scale * gain).astype(jnp.bfloat16)

def block_sum(hidden, weight):
    count, inner = hidden.shape
    width = inner // N_TP
    hidden_blocks = hidden.reshape(count, N_TP, width).transpose(1, 0, 2)
    weight_blocks = weight.reshape(N_TP, width, weight.shape[1])

    def add_block(total, pair):
        part = jnp.dot(pair[0], pair[1], preferred_element_type=jnp.float32).astype(jnp.bfloat16)
        part = lax.optimization_barrier(part)
        return (total + part.astype(jnp.float32), None)
    start = jnp.zeros((count, weight.shape[1]), jnp.float32)
    total, _ = lax.scan(add_block, start, (hidden_blocks, weight_blocks))
    return total

def half_ffn(stream, gain, gate_weight, up_weight, down_weight):
    normed = norm_rows(stream, gain)
    gate = jnp.dot(normed, gate_weight, preferred_element_type=jnp.float32)
    upward = jnp.dot(normed, up_weight, preferred_element_type=jnp.float32)
    hidden = (jax.nn.silu(gate) * upward).astype(jnp.bfloat16)
    branch = block_sum(hidden, down_weight)
    return (stream.astype(jnp.float32) + 0.5 * branch).astype(jnp.bfloat16)

def conv_mixer(stream, seqs, gain, conv_input, outer_gate, inner_gate, conv_taps, mixer_out):
    normed = norm_rows(stream, gain)
    conv_values = jnp.dot(normed, conv_input, preferred_element_type=jnp.float32)
    outer = jnp.dot(normed, outer_gate, preferred_element_type=jnp.float32)
    inner = jnp.dot(normed, inner_gate, preferred_element_type=jnp.float32)
    gated_input = (inner * conv_values).reshape(seqs, -1, conv_values.shape[1])
    one_back = jnp.pad(gated_input, ((0, 0), (1, 0), (0, 0)))[:, :-1]
    two_back = jnp.pad(gated_input, ((0, 0), (2, 0), (0, 0)))[:, :-2]
    convolved = conv_taps[0] * two_back + conv_taps[1] * one_back + conv_taps[2] * gated_input
    mixed = (outer * convolved.reshape(conv_values.shape)).astype(jnp.bfloat16)
    branch = block_sum(mixed, mixer_out)
    return (stream.astype(jnp.float32) + branch).astype(jnp.bfloat16)

def reference(tokens, first_gain, first_gate, first_up, first_down, mixer_gain, conv_input, outer_gate, inner_gate, conv_taps, mixer_out, second_gain, second_gate, second_up, second_down):
    seqs, length, width = tokens.shape
    stream = tokens.reshape(seqs * length, width)
    stream = half_ffn(stream, first_gain, first_gate, first_up, first_down)
    stream = conv_mixer(stream, seqs, mixer_gain, conv_input, outer_gate, inner_gate, conv_taps, mixer_out)
    stream = half_ffn(stream, second_gain, second_gate, second_up, second_down)
    return stream.reshape(seqs, length, width)
```

```python
import functools

import jax
import jax.numpy as jnp
from jax import lax
from jax.experimental import pallas as pl
from jax.experimental.pallas import tpu as pltpu
from jax.sharding import PartitionSpec as P

epsilon = 1e-05
MESH = pl.DeviceIdType.MESH
UP, DOWN, ACROSS = 0, 1, 2


def tile_of(columns):
    return 256 if columns % 256 == 0 else 128


def when(condition):
    return pl.when(condition)


def layer_kernel(n_fs, n_tp, seqs, length, n_late, *refs):
    tokens, first_gain, mixer_gain, second_gain, conv_taps = refs[:5]
    shards = refs[5:14]
    late_shard = refs[14]
    out_ref = refs[15]
    wholes = refs[16:25]
    late_whole, blocks, normed, hidden, partial, arrived = refs[25:31]
    (
        load_sem, send_sem, recv_sem, late_send, late_recv,
        gather_send, gather_recv, scatter_send, scatter_recv, token_sem,
    ) = refs[31:]
    n_early = len(shards)
    rows = seqs * length
    line = n_fs // 2

    me = lax.axis_index("fs")
    z, x = me // 2, lax.rem(me, 2)
    above, below, beside = me + 2, me - 2, me + 1 - 2 * x
    has_above, has_below = z + 1 < line, z >= 1
    t = lax.axis_index("tp")
    pair = t + 1 - 2 * lax.rem(t, 2)
    chips = n_tp // 2
    facing = [lax.rem(t + 2 * d, n_tp) for d in range(chips)]
    diagonal = [lax.rem(pair + 2 * d, n_tp) for d in range(chips)]
    others = range(1, chips)

    token_copy = pltpu.make_async_copy(tokens, blocks.at[0, t], token_sem)
    token_copy.start()
    loads = [
        pltpu.make_async_copy(shards[m], wholes[m].at[me], load_sem.at[m]) for m in range(n_early)
    ]
    depth = late_shard.shape[0] // n_late
    late_load = pltpu.make_async_copy(late_shard, late_whole.at[me], load_sem.at[n_early])
    for load in loads:
        load.start()
    late_load.start()

    barrier = pltpu.get_barrier_semaphore()

    def greet(axis, device):
        pl.semaphore_signal(barrier, inc=1, device_id={axis: device}, device_id_type=MESH)

    greet("tp", pair)
    for d in others:
        greet("tp", facing[d])
    greet("fs", beside)
    when(has_above)(lambda: greet("fs", above))
    when(has_below)(lambda: greet("fs", below))
    pl.semaphore_wait(
        barrier, chips + 1 + has_above.astype(jnp.int32) + has_below.astype(jnp.int32)
    )

    def early_copy(m, origin, way):
        return pltpu.make_async_remote_copy(
            src_ref=wholes[m].at[origin],
            dst_ref=wholes[m].at[origin],
            send_sem=send_sem.at[m, origin, way],
            recv_sem=recv_sem.at[m, origin],
            device_id={"fs": (above, below, beside)[way]},
            device_id_type=MESH,
        )

    def late_copy(k, origin, way):
        part = pl.ds(k * depth, depth)
        return pltpu.make_async_remote_copy(
            src_ref=late_whole.at[origin, part],
            dst_ref=late_whole.at[origin, part],
            send_sem=late_send.at[k, origin, way],
            recv_sem=late_recv.at[k, origin],
            device_id={"fs": (above, below, beside)[way]},
            device_id_type=MESH,
        )

    def early_own(m):
        loads[m].wait()
        early_copy(m, me, ACROSS).start()
        when(has_above)(lambda: early_copy(m, me, UP).start())
        when(has_below)(lambda: early_copy(m, me, DOWN).start())

    def early_step(m, step):
        @when(z >= step)
        def _():
            origin = me - 2 * step
            early_copy(m, origin, ACROSS).wait_recv()
            when(has_above)(lambda: early_copy(m, origin, UP).start())
            early_copy(m, origin, ACROSS).start()

        @when(z + step < line)
        def _():
            origin = me + 2 * step
            early_copy(m, origin, ACROSS).wait_recv()
            when(has_below)(lambda: early_copy(m, origin, DOWN).start())
            early_copy(m, origin, ACROSS).start()

    def early_across(m):
        for at in range(line):
            early_copy(m, 2 * at + 1 - x, ACROSS).wait_recv()

    def late_own(k):
        if k == 0:
            late_load.wait()
        late_copy(k, me, ACROSS).start()
        when(has_above)(lambda: late_copy(k, me, UP).start())
        when(has_below)(lambda: late_copy(k, me, DOWN).start())

    def late_across(k):
        late_copy(k, beside, ACROSS).wait_recv()
        when(has_above)(lambda: late_copy(k, beside, UP).start())
        when(has_below)(lambda: late_copy(k, beside, DOWN).start())

    def late_step(k, step):
        @when(z >= step)
        def _():
            for column in (me, beside):
                origin = column - 2 * step
                late_copy(k, origin, ACROSS).wait_recv()
                when(has_above)(functools.partial(lambda o: late_copy(k, o, UP).start(), origin))

        @when(z + step < line)
        def _():
            for column in (me, beside):
                origin = column + 2 * step
                late_copy(k, origin, ACROSS).wait_recv()
                when(has_below)(functools.partial(lambda o: late_copy(k, o, DOWN).start(), origin))

    def drain():
        for at in range(line):
            own_column = 2 * at + x
            for m in range(n_early):
                early_copy(m, own_column, ACROSS).wait_send()

            @when(jnp.logical_and(at <= z, has_above))
            def _():
                for m in range(n_early):
                    early_copy(m, own_column, UP).wait_send()
                for k in range(n_late):
                    for column in range(2):
                        late_copy(k, 2 * at + column, UP).wait_send()

            @when(jnp.logical_and(at >= z, has_below))
            def _():
                for m in range(n_early):
                    early_copy(m, own_column, DOWN).wait_send()
                for k in range(n_late):
                    for column in range(2):
                        late_copy(k, 2 * at + column, DOWN).wait_send()

        for k in range(n_late):
            late_copy(k, me, ACROSS).wait_send()

    def gather_copy(phase, block, way):
        target = pair if way == 0 or way >= chips else facing[way]
        return pltpu.make_async_remote_copy(
            src_ref=blocks.at[phase, block],
            dst_ref=blocks.at[phase, block],
            send_sem=gather_send.at[phase, way],
            recv_sem=gather_recv.at[phase, block],
            device_id={"tp": target},
            device_id_type=MESH,
        )

    def gather_start(phase):
        for d in others:
            gather_copy(phase, t, d).start()
        gather_copy(phase, t, 0).start()

    def gather_forward(phase):
        for d in others:
            gather_copy(phase, facing[d], d).wait_recv()
            gather_copy(phase, facing[d], chips + d - 1).start()

    def gather_finish(phase):
        gather_copy(phase, pair, 0).wait_recv()
        gather_copy(phase, t, 0).wait_send()
        for d in others:
            gather_copy(phase, diagonal[d], 0).wait_recv()
            gather_copy(phase, t, d).wait_send()
            gather_copy(phase, facing[d], chips + d - 1).wait_send()

    def scatter_copy(phase, way):
        block = diagonal[way] if way < chips else facing[way - chips + 1]
        target = pair if way < chips else facing[way - chips + 1]
        return pltpu.make_async_remote_copy(
            src_ref=partial.at[block],
            dst_ref=arrived.at[phase, way],
            send_sem=scatter_send.at[phase, way],
            recv_sem=scatter_recv.at[phase, way],
            device_id={"tp": target},
            device_id_type=MESH,
        )

    chunk = length // 3

    def row_loop(body):
        @pl.loop(0, rows // chunk)
        def _(i):
            body(pl.ds(pl.multiple_of(i * chunk, chunk), chunk))

    def scatter_start(phase):
        for d in others:
            scatter_copy(phase, d).start()
        scatter_copy(phase, 0).start()

    def scatter_middle(phase):
        for d in others:
            scatter_copy(phase, d).wait_recv()
            block = facing[d]

            def body(at):
                total = partial[block, at, :].astype(jnp.float32) + arrived[
                    phase, d, at, :
                ].astype(jnp.float32)
                partial[block, at, :] = total.astype(jnp.bfloat16)

            row_loop(body)
            scatter_copy(phase, chips + d - 1).start()

    def scatter_finish(phase, scale):
        scatter_copy(phase, 0).wait_recv()
        for d in others:
            scatter_copy(phase, chips + d - 1).wait_recv()

        def body(at):
            branch = partial[t, at, :].astype(jnp.float32)
            for way in [0] + [chips + d - 1 for d in others]:
                branch = branch + arrived[phase, way, at, :].astype(jnp.float32)
            value = (blocks[phase, t, at, :].astype(jnp.float32) + scale * branch).astype(
                jnp.bfloat16
            )
            if phase == 2:
                out_ref[at, :] = value
            else:
                blocks[phase + 1, t, at, :] = value

        row_loop(body)
        for way in range(2 * chips - 1):
            scatter_copy(phase, way).wait_send()

    width = tokens.shape[1]

    def norm(phase, gain):
        def body(at):
            values = [blocks[phase, b, at, :].astype(jnp.float32) for b in range(n_tp)]
            squares = sum(jnp.sum(v * v, axis=1, keepdims=True) for v in values)
            scale = lax.rsqrt(squares / (width * n_tp) + epsilon)
            for b, v in enumerate(values):
                cols = pl.ds(b * width, width)
                normed[at, cols] = (v * scale * gain[:, cols]).astype(jnp.bfloat16)

        row_loop(body)

    def times(at, m, cols):
        weight = wholes[m][:, :, cols]
        weight = weight.reshape(weight.shape[0] * weight.shape[1], weight.shape[2])
        return jnp.dot(normed[at, :], weight, preferred_element_type=jnp.float32)

    def ffn_inputs(gate, upward):
        tile = tile_of(wholes[gate].shape[2])

        @pl.loop(0, wholes[gate].shape[2] // tile)
        def _(n):
            cols = pl.ds(pl.multiple_of(n * tile, tile), tile)

            @pl.loop(0, seqs)
            def _(s):
                at = pl.ds(pl.multiple_of(s * length, length), length)
                g = times(at, gate, cols)
                g = g / (1.0 + jnp.exp(-g))
                hidden[at, cols] = (g * times(at, upward, cols)).astype(jnp.bfloat16)

    def project_down(whole):
        inner, piece = whole.shape[1:]
        per_block = width // piece

        @pl.loop(0, n_fs)
        def _(j):
            block = j // per_block
            cols = pl.ds(pl.multiple_of(lax.rem(j, per_block) * piece, piece), piece)

            @pl.loop(0, seqs)
            def _(s):
                at = pl.ds(pl.multiple_of(s * length, length), length)
                product = jnp.dot(
                    hidden[at, :inner], whole[j], preferred_element_type=jnp.float32
                )
                partial[block, at, cols] = product.astype(jnp.bfloat16)

    def mixer_inputs(conv_input, outer_gate, inner_gate):
        tile = tile_of(wholes[conv_input].shape[2])

        @pl.loop(0, wholes[conv_input].shape[2] // tile)
        def _(n):
            cols = pl.ds(pl.multiple_of(n * tile, tile), tile)
            taps = conv_taps[:, cols]
            position = lax.broadcasted_iota(jnp.int32, (length, tile), 0)

            @pl.loop(0, seqs)
            def _(s):
                at = pl.ds(pl.multiple_of(s * length, length), length)
                gated = times(at, inner_gate, cols) * times(at, conv_input, cols)
                one_back = jnp.where(position >= 1, pltpu.roll(gated, 1, 0), 0.0)
                two_back = jnp.where(position >= 2, pltpu.roll(gated, 2, 0), 0.0)
                convolved = taps[0:1] * two_back + taps[1:2] * one_back + taps[2:3] * gated
                hidden[at, cols] = (times(at, outer_gate, cols) * convolved).astype(jnp.bfloat16)

    units = [("e", 0), ("l", 0), ("e", 1), ("l", 1), ("e", 2), ("l", 2), ("e", 3), ("e", 4)]
    units += [("e", 5), ("e", 6), ("l", 3), ("e", 7), ("l", 4), ("e", 8)]
    ahead = 4

    def own(index):
        if index < len(units):
            kind, which = units[index]
            (early_own if kind == "e" else late_own)(which)

    def after_step(m, step):
        if m == 0 and step == 1:
            gather_forward(0)
        if m == 7:
            if step == 1:
                scatter_middle(1)
            if step == 2:
                scatter_finish(1, 1.0)
                gather_start(2)
            if step == 3:
                gather_forward(2)
        if m == 8 and step == 1:
            gather_finish(2)
            norm(2, second_gain)

    def after_unit(m):
        if m == 0:
            gather_finish(0)
            norm(0, first_gain)
        if m == 1:
            ffn_inputs(0, 1)
        if m == 2:
            project_down(wholes[2])
            scatter_start(0)
        if m == 3:
            scatter_middle(0)
        if m == 4:
            scatter_finish(0, 0.5)
            gather_start(1)
        if m == 5:
            gather_forward(1)
        if m == 6:
            gather_finish(1)
            norm(1, mixer_gain)
            mixer_inputs(3, 4, 5)
            project_down(wholes[6])
            scatter_start(1)
        if m == 8:
            ffn_inputs(7, 8)
            project_down(late_whole)
            scatter_start(2)
            scatter_middle(2)
            scatter_finish(2, 0.5)

    token_copy.wait()
    for index in range(ahead):
        own(index)
        if index == 0:
            gather_start(0)
    for index, (kind, which) in enumerate(units):
        if kind == "l":
            late_across(which)
        for step in range(1, line):
            if kind == "e":
                early_step(which, step)
                if step <= 3:
                    after_step(which, step)
            else:
                late_step(which, step)
        own(index + ahead)
        if kind == "e":
            early_across(which)
            after_unit(which)
    drain()


def on_device(n_fs, n_tp, *args):
    (
        tokens, first_gain, first_gate, first_up, first_down, mixer_gain, conv_input, outer_gate,
        inner_gate, conv_taps, mixer_out, second_gain, second_gate, second_up, second_down,
    ) = args
    seqs, length, width = tokens.shape
    rows, model = seqs * length, width * n_tp
    shards = (
        first_gate, first_up, first_down, conv_input, outer_gate, inner_gate, mixer_out,
        second_gate, second_up,
    )
    n_late = 5 if second_down.shape[0] % 80 == 0 else 1
    in_hbm = pl.BlockSpec(memory_space=pl.ANY)
    in_vmem = pl.BlockSpec(memory_space=pltpu.VMEM)
    half = jnp.bfloat16
    dma = pltpu.SemaphoreType.DMA
    scratch = [pltpu.VMEM((n_fs,) + shard.shape, half) for shard in shards]
    scratch += [
        pltpu.VMEM((n_fs,) + second_down.shape, half),
        pltpu.VMEM((3, n_tp, rows, width), half),
        pltpu.VMEM((rows, model), half),
        pltpu.VMEM((rows, first_gate.shape[1]), half),
        pltpu.VMEM((n_tp, rows, width), half),
        pltpu.VMEM((3, n_tp - 1, rows, width), half),
        dma((len(shards) + 1,)),
        dma((len(shards), n_fs, 3)),
        dma((len(shards), n_fs)),
        dma((n_late, n_fs, 3)),
        dma((n_late, n_fs)),
        dma((3, n_tp - 1)),
        dma((3, n_tp)),
        dma((3, n_tp - 1)),
        dma((3, n_tp - 1)),
        dma,
    ]
    flops = 2 * rows * model * (6 * first_gate.shape[1] + 4 * conv_input.shape[1])
    out = pl.pallas_call(
        functools.partial(layer_kernel, n_fs, n_tp, seqs, length, n_late),
        out_shape=jax.ShapeDtypeStruct((rows, width), half),
        in_specs=[in_hbm] + [in_vmem] * 4 + [in_hbm] * 10,
        out_specs=in_vmem,
        scratch_shapes=scratch,
        compiler_params=pltpu.CompilerParams(
            collective_id=0, has_side_effects=True, vmem_limit_bytes=67043328
        ),
        cost_estimate=pl.CostEstimate(flops=flops, bytes_accessed=0, transcendentals=0),
        name="whole_layer",
    )(
        tokens.reshape(rows, width),
        first_gain.reshape(1, model),
        mixer_gain.reshape(1, model),
        second_gain.reshape(1, model),
        conv_taps,
        *shards,
        second_down,
    )
    return out.reshape(seqs, length, width)


def solution(mesh):
    in_specs = (
        P("fs", None, "tp"),
        P(),
        P("fs", "tp"),
        P("fs", "tp"),
        P("tp", "fs"),
        P(),
        P("fs", "tp"),
        P("fs", "tp"),
        P("fs", "tp"),
        P(None, "tp"),
        P("tp", "fs"),
        P(),
        P("fs", "tp"),
        P("fs", "tp"),
        P("tp", "fs"),
    )
    body = functools.partial(on_device, mesh.shape["fs"], mesh.shape["tp"])
    return jax.shard_map(
        body, mesh=mesh, in_specs=in_specs, out_specs=P("fs", None, "tp"), check_vma=False
    )
```
